32 devices in a mesh: ep: 16 (over z, x, core), tp: 2 (over y).
Axes of the slice: x: 2, y: 2, z: 4, core: 2. Of those that a mesh axis runs over, the one named last changes fastest.
Arguments:
- hidden_in: bfloat16 [320, 2048], P('ep', 'tp'), may hold values from -32 to 32
- attn_gain: float32 [2048], replicated, may hold values from 0.1 to 1.9
- w_query: bfloat16 [256, 2048], P('tp'), may hold values from -0.125 to 0.125
- w_key: bfloat16 [256, 2048], P('tp'), may hold values from -0.125 to 0.125
- w_value: bfloat16 [256, 2048], P('tp'), may hold values from -0.125 to 0.125
- break_bias: float32 [4], P('tp'), may hold values from -9 to -3
- key_cache: bfloat16 [320, 256, 512], P('ep', 'tp'), may hold values from -6 to 6
- value_cache: bfloat16 [320, 256, 512], P('ep', 'tp'), may hold values from -8 to 8
- lengths: int32 [320], P('ep'), may hold values from 32 to 512
- w_out: bfloat16 [256, 2048], P('tp'), may hold values from -0.375 to 0.375
- ffn_gain: float32 [2048], replicated, may hold values from 0.1 to 1.9
- route_ids: int32 [320, 6], P('ep'), may hold values from 0 to 15, all different within a row; in each aligned block of 20 rows (0 to 19, 20 to 39, ...) at most 15 rows name the same one
- route_scores: float32 [320, 6], P('ep'), may hold values from 0.05 to 1
- expert_gate: bfloat16 [16, 2048, 512], P('ep', None, 'tp'), may hold values from -0.125 to 0.125
- expert_up: bfloat16 [16, 2048, 512], P('ep', None, 'tp'), may hold values from -0.125 to 0.125
- expert_down: bfloat16 [16, 512, 2048], P('ep', 'tp'), may hold values from -0.25 to 0.25
Outputs:
- hidden_out: bfloat16 [320, 2048], P('ep', 'tp')
- new_keys: bfloat16 [320, 256], P('ep', 'tp')
- new_values: bfloat16 [320, 256], P('ep', 'tp')
The draws below stay inside these ranges and needn't reach their ends.
Inputs may be any that keep to these rules, and one draw needn't show every extreme that they name: `route_ids`: each row names 6 distinct experts. Within each aligned block of 20 rows (the rows of one device) no expert is named more than 15 times, a bound that some block reaches.
All inputs are finite; a program needn't handle non-finite values.
Results may differ from the reference program's by a relative error of at most 0.0055.
Values may be sent and summed in bfloat16 or wider, within the bound.
A program may use at most 64 MiB of HBM per device.

```python
import math
import jax
import jax.numpy as jnp
import numpy as np
from jax import lax

D = 2048
HEADS = 4
HEAD_DIM = 64
WIDTH = 256
FF = 512
FF_DEV = 256
EXPERTS = 16
TOPK = 6
SEQ_DEV = 20
TOKENS = 320
CACHE = 512
CAP = 15
N_EP = 16
N_TP = 2


def draw_hidden_in(key, part):
    noise_key, row_key, col_key = jax.random.split(jax.random.fold_in(key, 11), 3)
    column = jnp.arange(D, dtype=jnp.float32) / D
    col_scale = 0.2 * 10.0 ** (column + 0.3 * jax.random.uniform(col_key, (D,), jnp.float32))
    row_scale = jax.random.uniform(row_key, (TOKENS, 1), jnp.float32, 0.5, 2.0)
    base = jnp.clip(jax.random.normal(noise_key, (TOKENS, D), jnp.float32), -4.0, 4.0)
    values = base * col_scale[None, :]
    return (values * row_scale).astype(jnp.bfloat16)


def draw_break_bias(key, part):
    bias_key = jax.random.fold_in(key, 23)
    values = jax.random.uniform(bias_key, (HEADS,), jnp.float32, -8.0, -3.0)
    return values.astype(jnp.float32)


def draw_value_cache(key, part):
    mean_key, noise_key = jax.random.split(jax.random.fold_in(key, 37), 2)
    center = jnp.clip(jax.random.normal(mean_key, (TOKENS, WIDTH, 1), jnp.float32), -4.0, 4.0)
    noise = jnp.clip(jax.random.normal(noise_key, (TOKENS, WIDTH, CACHE), jnp.float32), -4.0, 4.0)
    values = center + noise
    return values.astype(jnp.bfloat16)


def set_ends(array, stream_key, smallest, largest):
    index_at = [jax.random.randint(jax.random.fold_in(stream_key, axis), (), 0, length) for axis, length in enumerate(array.shape)]
    longest = array.shape.index(max(array.shape))
    next_to = index_at[:longest] + [(index_at[longest] + 1) % array.shape[longest]] + index_at[longest + 1:]
    return array.at[tuple(index_at)].set(smallest).at[tuple(next_to)].set(largest)


def steps_of(key, shape, cuts, smallest, largest):
    level = 1.0
    for dim, parts in cuts:
        heights = jax.random.uniform(jax.random.fold_in(jax.random.fold_in(key, 6), dim), (parts,), jnp.float32, smallest / len(cuts), largest / len(cuts))
        level = level * jnp.repeat(jnp.exp(heights), shape[dim] // parts).reshape((-1,) + (1,) * (len(shape) - 1 - dim))
    return level


def assign_block(key, own, number, rows, number_of, top, bound, skew):
    sequence = jax.random.permutation(key, number_of)
    crowded, usual = load_shares(number_of, rows * top, bound, skew, True), load_shares(number_of, rows * top, bound, skew, False)
    places = jnp.arange(number_of)

    def named(sizes, offset_by):
        used = int((sizes > 0).sum())
        fixed = max(1, used // 4)
        passed = fixed + (places - fixed + offset_by * (used - fixed)) % max(1, number_of - fixed)
        return jnp.zeros((number_of,), jnp.int32).at[sequence[jnp.where(places < fixed, places, passed)]].set(jnp.asarray(sizes, jnp.int32))

    sizes = jnp.where(number % 4 == 0, named(crowded, number // 4), named(usual, number - number // 4 - 1))
    mixed = jax.random.permutation(jax.random.fold_in(own, 3), number_of)
    giver, receiver = mixed[0:number_of // 2 * 2:2], mixed[1:number_of // 2 * 2:2]
    slack = jnp.minimum(sizes[giver] - 1, bound - sizes[receiver]) // 2
    slack = jnp.where((giver == sequence[0]) | (receiver == sequence[0]) | (sizes[receiver] == 0), 0, jnp.maximum(slack, 0))
    passed = jax.random.randint(jax.random.fold_in(own, 4), (number_of // 2,), 0, 1 << 20) % (slack + 1)
    sizes = sizes.at[giver].add(-passed).at[receiver].add(passed)
    members = jnp.searchsorted(jnp.cumsum(sizes), jnp.arange(rows * top), side="right").astype(jnp.int32)
    grid = members.reshape(top, rows).T
    grid = grid[jax.random.permutation(jax.random.fold_in(own, 1), rows)]
    offset_by = jax.random.randint(jax.random.fold_in(own, 2), (rows, 1), 0, top)
    return jnp.take_along_axis(grid, (jnp.arange(top)[None, :] + offset_by) % top, axis=1)


def load_shares(count, total, limit, lean, full):
    weights = [(1 << 20) // math.isqrt(standing ** lean) + 1 for standing in range(1, count + 1)]
    largest = limit if full else min(limit, max(-(-total // count), total * weights[0] // sum(weights)))
    least = 1 if total - largest >= count - 1 else 0
    holding, surplus = [largest] + [least] * (count - 1), total - largest - least * (count - 1)
    while surplus > 0:
        candidates = [i for i in range(1, count) if holding[i] < largest] or [i for i in range(1, count) if holding[i] < limit]
        whole, remaining = sum([weights[i] for i in candidates]), surplus
        for i in candidates:
            addition = min(limit - holding[i], max(1, remaining * weights[i] // whole), surplus)
            holding[i] = holding[i] + addition
            surplus = surplus - addition
    return np.array(holding)


def bell_draw(stream_key, dims, spread, bound, cuts=(), kind=jnp.bfloat16):
    entries = jax.random.normal(stream_key, dims, jnp.float32) * spread
    if len(cuts) > 0:
        entries = steps_of(stream_key, dims, cuts, -0.22, 0.18) * entries
    return jnp.clip(entries, min=-bound, max=bound).astype(kind)


def setup_inputs(seed: int = 0) -> dict:
    key_of = jax.random.split(jax.random.key(seed), 17)
    hidden_in = draw_hidden_in(jax.random.fold_in(key_of[16], 71), 0)
    attn_gain = jnp.clip(1.0 + 0.18 * jax.random.normal(key_of[1], (D,), jnp.float32), 0.1, 1.9)
    w_query = bell_draw(key_of[2], (WIDTH, D), D ** -0.5, 0.125, ((0, 2),))
    w_key = bell_draw(key_of[3], (WIDTH, D), D ** -0.5, 0.125, ((0, 2),))
    w_value = bell_draw(key_of[4], (WIDTH, D), D ** -0.5, 0.125, ((0, 2),))
    break_bias = draw_break_bias(jax.random.fold_in(key_of[16], 71), 0)
    key_cache = bell_draw(key_of[6], (TOKENS, WIDTH, CACHE), 1.0, 6.0, ((0, 16), (1, 2)))
    value_cache = draw_value_cache(jax.random.fold_in(key_of[16], 71), 0)
    lengths = set_ends(jax.random.randint(key_of[8], (TOKENS,), CACHE // 16, CACHE + 1), jax.random.fold_in(key_of[8], 1), CACHE // 16, CACHE).astype(jnp.int32)
    w_out = bell_draw(key_of[9], (WIDTH, D), WIDTH ** -0.5, 0.375, ((0, 2),))
    ffn_gain = jnp.clip(1.0 + 0.18 * jax.random.normal(key_of[10], (D,), jnp.float32), 0.1, 1.9)
    route_ids_keys = jax.random.split(jax.random.fold_in(key_of[11], 1), TOKENS // SEQ_DEV)
    route_ids_turns = jax.random.permutation(jax.random.fold_in(key_of[11], 3), TOKENS // SEQ_DEV)
    route_ids = jax.vmap(lambda own, number: assign_block(jax.random.fold_in(key_of[11], 2), own, number, SEQ_DEV, EXPERTS, TOPK, CAP, 2))(route_ids_keys, route_ids_turns).reshape((TOKENS, TOPK))
    route_scores = jnp.clip(0.05 + 0.95 * jax.random.uniform(key_of[12], (TOKENS, TOPK), jnp.float32) ** steps_of(key_of[12], (TOKENS, TOPK), ((0, 16),), -0.2, 0.2), 0.05, 1.0)
    expert_gate = bell_draw(key_of[13], (EXPERTS, D, FF), D ** -0.5, 0.125, ((0, 16), (2, 2)))
    expert_up = bell_draw(key_of[14], (EXPERTS, D, FF), D ** -0.5, 0.125, ((0, 16), (2, 2)))
    expert_down = bell_draw(key_of[15], (EXPERTS, FF, D), FF ** -0.5, 0.25, ((0, 16), (1, 2)))
    return dict(hidden_in=hidden_in, attn_gain=attn_gain, w_query=w_query, w_key=w_key, w_value=w_value, break_bias=break_bias, key_cache=key_cache, value_cache=value_cache, lengths=lengths, w_out=w_out, ffn_gain=ffn_gain, route_ids=route_ids, route_scores=route_scores, expert_gate=expert_gate, expert_up=expert_up, expert_down=expert_down)


norm_eps = 1e-06

def rms_norm(row_values, norm_gain):
    values = row_values.astype(jnp.float32)
    inverse_rms = lax.rsqrt(lax.optimization_barrier(jnp.mean(values * values, axis=-1, keepdims=True)) + norm_eps)
    return (values * inverse_rms * norm_gain).astype(jnp.bfloat16)

def project_rows(normed, weight):
    return lax.dot_general(normed, weight, (((1,), (1,)), ((), ())), preferred_element_type=jnp.float32).astype(jnp.bfloat16)

def stick_breaking(queries, key_block, value_block, lengths, break_bias):
    head_count = break_bias.shape[0]
    q_heads = queries.reshape(queries.shape[0], head_count, -1).astype(jnp.float32)
    k_heads = key_block.reshape(key_block.shape[0], head_count, -1, key_block.shape[2]).astype(jnp.float32)
    v_heads = value_block.reshape(value_block.shape[0], head_count, -1, value_block.shape[2]).astype(jnp.float32)
    logit = jnp.einsum('shd,shdl->shl', q_heads, k_heads) * HEAD_DIM ** (-0.5) + break_bias[None, :, None]
    position = jnp.arange(key_block.shape[2], dtype=jnp.int32)
    visible = (position[None, :] < lengths[:, None])[:, None, :]
    log_keep = jnp.where(visible, jax.nn.log_sigmoid(-logit), 0.0)
    later_sum = lax.cumsum(log_keep, axis=2, reverse=True) - log_keep
    stick = jnp.where(visible, jnp.exp(jax.nn.log_sigmoid(logit) + later_sum), 0.0).astype(jnp.bfloat16)
    attended = jnp.einsum('shl,shdl->shd', stick.astype(jnp.float32), v_heads)
    return attended.reshape(queries.shape[0], -1).astype(jnp.bfloat16)

def slot_ranks(route_ids):
    block_ids = route_ids.reshape(-1, SEQ_DEV * TOPK)
    expert_iota = jnp.arange(EXPERTS, dtype=jnp.int32)
    onehot = (block_ids[:, :, None] == expert_iota[None, None, :]).astype(jnp.int32)
    earlier = jnp.cumsum(onehot, axis=1) - onehot
    return lax.optimization_barrier(jnp.sum(earlier * onehot, axis=2)).reshape(route_ids.shape).astype(jnp.int32)

def one_expert(operands):
    rows_in, gate_w, up_w, down_w = operands
    gate_act = jnp.dot(rows_in, gate_w, preferred_element_type=jnp.float32)
    up_act = jnp.dot(rows_in, up_w, preferred_element_type=jnp.float32)
    hidden = (jax.nn.silu(gate_act) * up_act).astype(jnp.bfloat16)
    blocks = hidden.reshape(hidden.shape[0], N_TP, FF_DEV).astype(jnp.float32)
    down_blocks = down_w.reshape(N_TP, FF_DEV, D).astype(jnp.float32)
    partial_value = jnp.einsum('rtf,tfd->trd', blocks, down_blocks).astype(jnp.bfloat16)
    partial_value = lax.optimization_barrier(partial_value)
    return lax.optimization_barrier(jnp.sum(partial_value.astype(jnp.float32), axis=0)).astype(jnp.bfloat16)

def reference(hidden_in, attn_gain, w_query, w_key, w_value, break_bias, key_cache, value_cache, lengths, w_out, ffn_gain, route_ids, route_scores, expert_gate, expert_up, expert_down):
    normed_attn = rms_norm(hidden_in, attn_gain)
    queries = project_rows(normed_attn, w_query)
    new_keys = project_rows(normed_attn, w_key)
    new_values = project_rows(normed_attn, w_value)
    attended = stick_breaking(queries, key_cache, value_cache, lengths, break_bias)
    mixer_out = jnp.dot(attended, w_out, preferred_element_type=jnp.float32)
    residual = (hidden_in.astype(jnp.float32) + mixer_out).astype(jnp.bfloat16)
    normed_ffn = rms_norm(residual, ffn_gain)
    ranks = slot_ranks(route_ids)
    token_index = jnp.arange(TOKENS, dtype=jnp.int32)
    block_index = token_index // SEQ_DEV
    target = (route_ids * (N_EP * CAP) + block_index[:, None] * CAP + ranks).astype(jnp.int32)
    table = jnp.full((EXPERTS * N_EP * CAP,), TOKENS, jnp.int32)
    table = table.at[target.reshape(-1)].set(jnp.repeat(token_index, TOPK))
    padded = jnp.concatenate([normed_ffn, jnp.zeros((1, D), jnp.bfloat16)], axis=0)
    expert_rows = padded[table].reshape(EXPERTS, N_EP * CAP, D)
    results = lax.map(one_expert, (expert_rows, expert_gate, expert_up, expert_down))
    flat_results = results.reshape(EXPERTS * N_EP * CAP, D)
    picked = flat_results[target].astype(jnp.float32)
    route_weight = route_scores / lax.optimization_barrier(jnp.sum(route_scores, axis=1, keepdims=True))
    expert_mix = lax.optimization_barrier(jnp.sum(picked * route_weight[:, :, None], axis=1))
    hidden_out = (residual.astype(jnp.float32) + expert_mix).astype(jnp.bfloat16)
    return (hidden_out, new_keys, new_values)
```

```python
import functools

import jax
import jax.numpy as jnp
from jax import lax
from jax.experimental import pallas as pl
from jax.experimental.pallas import tpu as pltpu
from jax.sharding import PartitionSpec as P

HEAD_DIM = 64


norm_eps = 1e-06


def rms_norm(row_values, norm_gain):
    values = row_values.astype(jnp.float32)
    inverse_rms = lax.rsqrt(jnp.mean(values * values, axis=-1, keepdims=True) + norm_eps)
    return (values * inverse_rms * norm_gain).astype(jnp.bfloat16)


def project_rows(normed, weight):
    return lax.dot_general(
        normed, weight, (((1,), (1,)), ((), ())), preferred_element_type=jnp.float32
    ).astype(jnp.bfloat16)


def sum_later(values):
    span = values.shape[-1]
    flat = values.reshape(-1, span)
    row = lax.broadcasted_iota(jnp.int32, (span, span), 0)
    col = lax.broadcasted_iota(jnp.int32, (span, span), 1)
    later = (row > col).astype(jnp.bfloat16)
    total, rest = 0.0, flat
    for _ in range(3):
        term = rest.astype(jnp.bfloat16)
        rest = rest - term.astype(jnp.float32)
        total = total + jnp.dot(term, later, preferred_element_type=jnp.float32)
    return total.reshape(values.shape)


def stick_breaking(queries, key_block, value_block, lengths, break_bias):
    head_count = break_bias.shape[0]
    q_heads = queries.reshape(queries.shape[0], head_count, HEAD_DIM)
    k_heads = key_block.reshape(key_block.shape[0], head_count, HEAD_DIM, key_block.shape[2])
    v_heads = value_block.reshape(value_block.shape[0], head_count, HEAD_DIM, value_block.shape[2])
    logit = jnp.einsum("shd,shdl->shl", q_heads, k_heads, preferred_element_type=jnp.float32)
    logit = logit * HEAD_DIM ** (-0.5) + break_bias[None, :, None]
    position = jnp.arange(key_block.shape[2], dtype=jnp.int32)
    visible = (position[None, :] < lengths[:, None])[:, None, :]
    log_keep = jnp.where(visible, jax.nn.log_sigmoid(-logit), 0.0)
    later_sum = sum_later(log_keep)
    stick = jnp.where(visible, jnp.exp(jax.nn.log_sigmoid(logit) + later_sum), 0.0).astype(
        jnp.bfloat16
    )
    attended = jnp.einsum("shl,shdl->shd", stick, v_heads, preferred_element_type=jnp.float32)
    return attended.reshape(queries.shape[0], -1).astype(jnp.bfloat16)


def shards(
    hidden_in,
    attn_gain,
    w_query,
    w_key,
    w_value,
    break_bias,
    key_cache,
    value_cache,
    lengths,
    w_out,
    ffn_gain,
    route_ids,
    route_scores,
    expert_gate,
    expert_up,
    expert_down,
):
    gathered = lax.all_gather(hidden_in, "tp", axis=1, tiled=True)
    full_width = gathered.shape[1]
    slice_width = hidden_in.shape[1]
    offset = lax.axis_index("tp") * slice_width
    normed_attn = rms_norm(gathered, attn_gain)
    queries = project_rows(normed_attn, w_query)
    new_keys = project_rows(normed_attn, w_key)
    new_values = project_rows(normed_attn, w_value)
    attended = stick_breaking(queries, key_cache, value_cache, lengths, break_bias)
    partial_out = jnp.dot(attended, w_out, preferred_element_type=jnp.float32)
    mixer_part = lax.psum_scatter(partial_out, "tp", scatter_dimension=1, tiled=True)
    residual = (hidden_in.astype(jnp.float32) + mixer_part).astype(jnp.bfloat16)
    resid_values = residual.astype(jnp.float32)
    square_total = lax.psum(jnp.sum(resid_values * resid_values, axis=1), "tp")
    inverse_rms = lax.rsqrt(square_total / full_width + norm_eps)
    gain_part = lax.dynamic_slice_in_dim(ffn_gain, offset, slice_width)
    normed_part = (resid_values * inverse_rms[:, None] * gain_part[None, :]).astype(jnp.bfloat16)
    seq_count = hidden_in.shape[0]
    route_count = route_ids.shape[1]
    local_experts = expert_gate.shape[0]
    experts = local_experts * lax.axis_size("ep")
    capacity = min(seq_count, max(2, 2 * seq_count * route_count // experts))
    flat_ids = route_ids.reshape(-1)
    expert_iota = jnp.arange(experts, dtype=jnp.int32)
    onehot = (flat_ids[:, None] == expert_iota[None, :]).astype(jnp.int32)
    earlier = jnp.cumsum(onehot, axis=0) - onehot
    slot_index = flat_ids * capacity + jnp.sum(earlier * onehot, axis=1)
    slot_iota = jnp.arange(experts * capacity, dtype=jnp.int32)
    placement = (slot_index[:, None] == slot_iota[None, :]).astype(jnp.bfloat16)
    repeated = jnp.repeat(normed_part, route_count, axis=0)
    outgoing = jnp.einsum("ke,kd->ed", placement, repeated, preferred_element_type=jnp.float32)
    full_rows = lax.all_gather(
        lax.all_to_all(
            outgoing.astype(jnp.bfloat16).reshape(experts, capacity, normed_part.shape[1]),
            "ep",
            split_axis=0,
            concat_axis=0,
            tiled=True,
        ),
        "tp",
        axis=2,
        tiled=True,
    )
    senders = full_rows.shape[0] // local_experts
    grouped = full_rows.reshape(senders, local_experts, full_rows.shape[1], full_rows.shape[2])
    gate_act = jnp.einsum(
        "secd,edf->secf", grouped, expert_gate, preferred_element_type=jnp.float32
    )
    up_act = jnp.einsum("secd,edf->secf", grouped, expert_up, preferred_element_type=jnp.float32)
    hidden = (jax.nn.silu(gate_act) * up_act).astype(jnp.bfloat16)
    partial_value = jnp.einsum(
        "secf,efd->secd", hidden, expert_down, preferred_element_type=jnp.float32
    )
    partial_value = partial_value.astype(jnp.bfloat16)
    summed = lax.psum_scatter(
        partial_value.astype(jnp.float32).astype(jnp.bfloat16),
        "tp",
        scatter_dimension=3,
        tiled=True,
    )
    summed = summed.reshape(senders * local_experts, summed.shape[2], summed.shape[3])
    returned = lax.all_to_all(summed, "ep", split_axis=0, concat_axis=0, tiled=True)
    flat_back = returned.reshape(experts * capacity, returned.shape[2])
    picked = jnp.take(flat_back, slot_index, axis=0)
    picked = picked.astype(jnp.float32).reshape(seq_count, route_count, slice_width)
    route_weight = route_scores / jnp.sum(route_scores, axis=1, keepdims=True)
    expert_mix = jnp.sum(picked * route_weight[:, :, None], axis=1)
    hidden_out = (residual.astype(jnp.float32) + expert_mix).astype(jnp.bfloat16)
    return (hidden_out, new_keys, new_values)


def experts_kernel(
    sizes,
    part_ref,
    hid_ref,
    gain_ref,
    wts_ref,
    gate_hbm,
    up_hbm,
    down_hbm,
    out_ref,
    gate_w,
    up_w,
    down_w,
    part_in,
    resid,
    rows,
    own,
    for_sib,
    from_sib,
    stage_a,
    recv_a,
    stage_b,
    recv_b,
    stage_c,
    recv_c,
    stage_d,
    recv_d,
    load_sem,
    pair_send,
    pair_recv,
    z_send,
    z_recv,
    two_send,
    two_recv,
    three_send,
    three_recv,
    sib_send,
    sib_recv,
    red_send,
    red_recv,
):
    live, padded, zs, width, half, experts = sizes
    live = live + -live % 8
    quarter = half // 2
    ep = lax.axis_index("ep")
    y = lax.axis_index("tp")
    c = lax.rem(ep, 2)
    x = lax.rem(ep // 2, 2)
    z = ep // 4

    def device(zi, xi, ci, yi):
        return {"ep": zi * 4 + xi * 2 + ci, "tp": yi}

    sibling = device(z, x, 1 - c, y)
    across_y = device(z, x, c, 1 - y)
    across_x = device(z, 1 - x, c, y)
    axis_two = device(z, x + (1 - c) * (1 - 2 * x), c, y + c * (1 - 2 * y))
    axis_three = device(z, x + c * (1 - 2 * x), c, y + (1 - c) * (1 - 2 * y))

    loads = [
        pltpu.make_async_copy(gate_hbm.at[0], gate_w, load_sem.at[0]),
        pltpu.make_async_copy(up_hbm.at[0], up_w, load_sem.at[1]),
        pltpu.make_async_copy(down_hbm.at[0], down_w, load_sem.at[2]),
    ]
    for load in loads:
        load.start()

    barrier = pltpu.get_barrier_semaphore()
    partners = [sibling, across_y, across_x] + [
        device(lax.rem(z + d, zs), x, c, y) for d in range(1, zs)
    ]
    for partner in partners:
        pl.semaphore_signal(
            barrier, inc=1, device_id=partner, device_id_type=pl.DeviceIdType.MESH
        )
    pl.semaphore_wait(barrier, len(partners))

    pending = []

    def send(src, dst, send_sem, recv_sem, target):
        copy = pltpu.make_async_remote_copy(
            src_ref=src,
            dst_ref=dst,
            send_sem=send_sem,
            recv_sem=recv_sem,
            device_id=target,
            device_id_type=pl.DeviceIdType.MESH,
        )
        copy.start()
        pending.append(copy)
        return copy

    first = send(part_ref, part_in, pair_send.at[0], pair_recv.at[0], across_y)
    first.wait_recv()
    values = (hid_ref[...].astype(jnp.float32) + (part_ref[...] + part_in[...])).astype(
        jnp.bfloat16
    )
    values = values.astype(jnp.float32)
    resid[...] = values
    inverse = lax.rsqrt(jnp.sum(values * values, axis=1, keepdims=True) / width + norm_eps)
    mine = pl.ds(pl.multiple_of(y * half, half), half)
    normed = resid[:, mine] * inverse * gain_ref[:, mine]
    rows[y, x, z, c, :, :half] = normed.astype(jnp.bfloat16)
    rows[y, x, z, c, :, half:] = wts_ref[...]

    def block(yi, xi, zi):
        return rows.at[yi, xi, zi, c, pl.ds(0, live), :]

    def share(where, slot, send_sem, recv_sem, target):
        ref = block(*where)
        return send(ref, ref, send_sem.at[slot], recv_sem.at[slot], target)

    from_z, from_two, from_three, from_core = [], [], [], []
    me = (y, x, z)
    for d in range(1, zs):
        from_z.append(
            share(me, d - 1, z_send, z_recv, device(lax.rem(z + d, zs), x, c, y))
        )
    for d in range(zs):
        if d > 0:
            from_z[d - 1].wait_recv()
        where = (y, x, lax.rem(z - d + zs, zs))
        from_two.append(share(where, d, two_send, two_recv, axis_two))
        from_three.append(share(where, d, three_send, three_recv, axis_three))
        from_core.append(share(where, d, sib_send, sib_recv, sibling))
    x_two, y_two = x + (1 - c) * (1 - 2 * x), y + c * (1 - 2 * y)
    for d in range(zs):
        from_two[d].wait_recv()
        where = (y_two, x_two, lax.rem(z - d + zs, zs))
        from_three.append(share(where, zs + d, three_send, three_recv, axis_three))
        from_core.append(share(where, zs + d, sib_send, sib_recv, sibling))
    x_three, y_three = x + c * (1 - 2 * x), y + (1 - c) * (1 - 2 * y)
    for d in range(2 * zs):
        from_three[d].wait_recv()
        zi = lax.rem(z - d + 2 * zs, zs)
        where = (y_three, x_three, zi) if d < zs else (1 - y, 1 - x, zi)
        from_core.append(share(where, 2 * zs + d, sib_send, sib_recv, sibling))
    for copy in from_core:
        copy.wait_recv()
    for load in loads:
        load.wait()

    count = 4 * zs * padded
    gate_act, up_act = 0.0, 0.0
    for yi in range(2):
        taken = rows[yi, :, :, :, :, :half].reshape(count, half)
        depth = slice(yi * half, (yi + 1) * half)
        gate_act += jnp.dot(taken, gate_w[depth], preferred_element_type=jnp.float32)
        up_act += jnp.dot(taken, up_w[depth], preferred_element_type=jnp.float32)
    hidden = (jax.nn.silu(gate_act) * up_act).astype(jnp.bfloat16)
    coded = rows[0, :, :, :, :, half:].reshape(count, -1).astype(jnp.float32)
    lane = lax.broadcasted_iota(jnp.int32, coded.shape, 1)
    named = (lane == ep) | (lane == ep + experts)
    weight = jnp.sum(jnp.where(named, coded, 0.0), axis=1, keepdims=True)

    def piece(yi, ci):
        columns = pl.ds(pl.multiple_of(yi * half + ci * quarter, quarter), quarter)
        result = jnp.dot(hidden, down_w[:, columns], preferred_element_type=jnp.float32)
        return (result * weight).reshape(2, zs, 2, padded, quarter)

    halves = []
    for yi in range(2):
        for_sib[yi] = piece(yi, 1 - c).astype(jnp.bfloat16)
        halves.append(
            send(for_sib.at[yi], from_sib.at[yi], red_send.at[yi], red_recv.at[yi], sibling)
        )
    for yi in range(2):
        own[yi] = piece(yi, c)
    for copy in halves:
        copy.wait_recv()

    one = y + c * (x - y)
    two = x + c * (y - x)

    def summed(fi, si):
        yi, xi = fi + c * (si - fi), si + c * (fi - si)
        return own[yi, xi] + from_sib[yi, xi].astype(jnp.float32)

    for si in range(2):
        stage_a[si] = summed(1 - one, si).astype(jnp.bfloat16)
    to_first = send(stage_a, recv_a, red_send.at[2], red_recv.at[2], axis_three)
    to_first.wait_recv()
    stage_b[...] = (summed(one, 1 - two) + recv_a[1 - two].astype(jnp.float32)).astype(
        jnp.bfloat16
    )
    to_second = send(stage_b, recv_b, red_send.at[3], red_recv.at[3], axis_two)
    kept = summed(one, two) + recv_a[two].astype(jnp.float32)
    to_second.wait_recv()
    own[0, 0] = kept + recv_b[...].astype(jnp.float32)
    stage_c[...] = own[0, 0].astype(jnp.bfloat16)
    along_z = []
    for d in range(1, zs):
        zi = lax.rem(z + d, zs)
        along_z.append(
            send(
                stage_c.at[zi, :, pl.ds(0, live), :],
                recv_c.at[d - 1, :, pl.ds(0, live), :],
                red_send.at[3 + d],
                red_recv.at[3 + d],
                device(zi, x, c, y),
            )
        )
    total = own[0, 0, z]
    for d in range(1, zs):
        along_z[d - 1].wait_recv()
        total = total + recv_c[d - 1].astype(jnp.float32)
    stage_d[...] = total
    last = send(
        stage_d.at[1 - c], recv_d, red_send.at[3 + zs], red_recv.at[3 + zs], sibling
    )
    near = pl.multiple_of(c * quarter, quarter)
    far = pl.multiple_of((1 - c) * quarter, quarter)
    base = pl.multiple_of(y * half, half)
    out_ref[:, pl.ds(near, quarter)] = (
        resid[:, pl.ds(pl.multiple_of(base + near, quarter), quarter)] + stage_d[c]
    ).astype(out_ref.dtype)
    last.wait_recv()
    out_ref[:, pl.ds(far, quarter)] = (
        resid[:, pl.ds(pl.multiple_of(base + far, quarter), quarter)] + recv_d[...]
    ).astype(out_ref.dtype)
    for copy in pending:
        copy.wait_send()


def expert_layer(
    partial_out, gathered, ffn_gain, coded, expert_gate, expert_up, expert_down, live, ep_size
):
    padded, width = partial_out.shape
    half = width // 2
    zs = ep_size // 4
    blocks = (2, zs, 2, padded, half // 2)
    bf16, f32 = jnp.bfloat16, jnp.float32
    vmem = pl.BlockSpec(memory_space=pltpu.VMEM)
    hbm = pl.BlockSpec(memory_space=pl.ANY)
    dma = pltpu.SemaphoreType.DMA
    sizes = (live, padded, zs, width, half, ep_size)
    return pl.pallas_call(
        functools.partial(experts_kernel, sizes),
        out_shape=jax.ShapeDtypeStruct((padded, half), bf16),
        in_specs=[vmem] * 4 + [hbm] * 3,
        out_specs=vmem,
        scratch_shapes=[
            pltpu.VMEM(expert_gate.shape[1:], bf16),
            pltpu.VMEM(expert_up.shape[1:], bf16),
            pltpu.VMEM(expert_down.shape[1:], bf16),
            pltpu.VMEM((padded, width), f32),
            pltpu.VMEM((padded, width), f32),
            pltpu.VMEM((2, 2, zs, 2, padded, half + coded.shape[1]), bf16),
            pltpu.VMEM((2,) + blocks, f32),
            pltpu.VMEM((2,) + blocks, bf16),
            pltpu.VMEM((2,) + blocks, bf16),
            pltpu.VMEM(blocks, bf16),
            pltpu.VMEM(blocks, bf16),
            pltpu.VMEM(blocks[1:], bf16),
            pltpu.VMEM(blocks[1:], bf16),
            pltpu.VMEM(blocks[1:], bf16),
            pltpu.VMEM((zs - 1,) + blocks[2:], bf16),
            pltpu.VMEM(blocks[2:], f32),
            pltpu.VMEM(blocks[3:], f32),
            dma((3,)),
            dma((1,)),
            dma((1,)),
            dma((zs - 1,)),
            dma((zs - 1,)),
            dma((zs,)),
            dma((zs,)),
            dma((2 * zs,)),
            dma((2 * zs,)),
            dma((4 * zs,)),
            dma((4 * zs,)),
            dma((4 + zs,)),
            dma((4 + zs,)),
        ],
        compiler_params=pltpu.CompilerParams(
            collective_id=0, has_side_effects=True, vmem_limit_bytes=60 * 1024 * 1024
        ),
    )(partial_out, gathered, ffn_gain, coded, expert_gate, expert_up, expert_down)


def dense_shards(
    hidden_in,
    attn_gain,
    w_query,
    w_key,
    w_value,
    break_bias,
    key_cache,
    value_cache,
    lengths,
    w_out,
    ffn_gain,
    route_ids,
    route_scores,
    expert_gate,
    expert_up,
    expert_down,
):
    gathered = lax.all_gather(hidden_in, "tp", axis=1, tiled=True)
    normed_attn = rms_norm(gathered, attn_gain)
    queries = project_rows(normed_attn, w_query)
    new_keys = project_rows(normed_attn, w_key)
    new_values = project_rows(normed_attn, w_value)
    attended = stick_breaking(queries, key_cache, value_cache, lengths, break_bias)
    live = hidden_in.shape[0]
    extra = ((0, -live % 16), (0, 0))
    partial_out = jnp.dot(jnp.pad(attended, extra), w_out, preferred_element_type=jnp.float32)
    experts = lax.axis_size("ep")
    route_weight = route_scores / jnp.sum(route_scores, axis=1, keepdims=True)
    named = route_ids[:, :, None] == jnp.arange(experts, dtype=jnp.int32)[None, None, :]
    dense = jnp.sum(jnp.where(named, route_weight[:, :, None], 0.0), axis=1)
    high = lax.reduce_precision(dense, 8, 7)
    coded = jnp.concatenate([high, dense - high], axis=1).astype(jnp.bfloat16)
    coded = jnp.pad(coded, (extra[0], (0, -coded.shape[1] % 128)))
    hidden_out = expert_layer(
        partial_out,
        jnp.pad(gathered, extra),
        ffn_gain[None, :],
        coded,
        expert_gate,
        expert_up,
        expert_down,
        live,
        experts,
    )
    return (hidden_out[:live], new_keys, new_values)


def solution(mesh):
    ep_size, tp_size = mesh.shape["ep"], mesh.shape["tp"]
    fits = tp_size == 2 and ep_size % 4 == 0 and 8 <= ep_size <= 16
    body = dense_shards if fits else shards
    return jax.shard_map(
        body,
        mesh=mesh,
        in_specs=(
            P("ep", "tp"),
            P(),
            P("tp", None),
            P("tp", None),
            P("tp", None),
            P("tp"),
            P("ep", "tp", None),
            P("ep", "tp", None),
            P("ep"),
            P("tp", None),
            P(),
            P("ep", None),
            P("ep", None),
            P("ep", None, "tp"),
            P("ep", None, "tp"),
            P("ep", "tp", None),
        ),
        out_specs=(P("ep", "tp"), P("ep", "tp"), P("ep", "tp")),
        check_vma=False,
    )
```

```python
import functools

import jax
import jax.numpy as jnp
from jax import lax
from jax.experimental import pallas as pl
from jax.experimental.pallas import tpu as pltpu
from jax.sharding import PartitionSpec as P

HEAD_DIM = 64


norm_eps = 1e-06


def rms_norm(row_values, norm_gain):
    values = row_values.astype(jnp.float32)
    inverse_rms = lax.rsqrt(jnp.mean(values * values, axis=-1, keepdims=True) + norm_eps)
    return (values * inverse_rms * norm_gain).astype(jnp.bfloat16)


def project_rows(normed, weight):
    return lax.dot_general(
        normed, weight, (((1,), (1,)), ((), ())), preferred_element_type=jnp.float32
    ).astype(jnp.bfloat16)


def stick_breaking(queries, key_block, value_block, lengths, break_bias):
    head_count = break_bias.shape[0]
    q_heads = queries.reshape(queries.shape[0], head_count, HEAD_DIM)
    k_heads = key_block.reshape(key_block.shape[0], head_count, HEAD_DIM, key_block.shape[2])
    v_heads = value_block.reshape(value_block.shape[0], head_count, HEAD_DIM, value_block.shape[2])
    logit = jnp.einsum("shd,shdl->shl", q_heads, k_heads, preferred_element_type=jnp.float32)
    logit = logit * HEAD_DIM ** (-0.5) + break_bias[None, :, None]
    position = jnp.arange(key_block.shape[2], dtype=jnp.int32)
    visible = (position[None, :] < lengths[:, None])[:, None, :]
    log_keep = jnp.where(visible, jax.nn.log_sigmoid(-logit), 0.0)
    later_sum = lax.cumsum(log_keep, axis=2, reverse=True) - log_keep
    stick = jnp.where(visible, jnp.exp(jax.nn.log_sigmoid(logit) + later_sum), 0.0).astype(
        jnp.bfloat16
    )
    attended = jnp.einsum("shl,shdl->shd", stick, v_heads, preferred_element_type=jnp.float32)
    return attended.reshape(queries.shape[0], -1).astype(jnp.bfloat16)


def shards(
    hidden_in,
    attn_gain,
    w_query,
    w_key,
    w_value,
    break_bias,
    key_cache,
    value_cache,
    lengths,
    w_out,
    ffn_gain,
    route_ids,
    route_scores,
    expert_gate,
    expert_up,
    expert_down,
):
    gathered = lax.all_gather(hidden_in, "tp", axis=1, tiled=True)
    full_width = gathered.shape[1]
    slice_width = hidden_in.shape[1]
    offset = lax.axis_index("tp") * slice_width
    normed_attn = rms_norm(gathered, attn_gain)
    queries = project_rows(normed_attn, w_query)
    new_keys = project_rows(normed_attn, w_key)
    new_values = project_rows(normed_attn, w_value)
    attended = stick_breaking(queries, key_cache, value_cache, lengths, break_bias)
    partial_out = jnp.dot(attended, w_out, preferred_element_type=jnp.float32)
    mixer_part = lax.psum_scatter(partial_out, "tp", scatter_dimension=1, tiled=True)
    residual = (hidden_in.astype(jnp.float32) + mixer_part).astype(jnp.bfloat16)
    resid_values = residual.astype(jnp.float32)
    square_total = lax.psum(jnp.sum(resid_values * resid_values, axis=1), "tp")
    inverse_rms = lax.rsqrt(square_total / full_width + norm_eps)
    gain_part = lax.dynamic_slice_in_dim(ffn_gain, offset, slice_width)
    normed_part = (resid_values * inverse_rms[:, None] * gain_part[None, :]).astype(jnp.bfloat16)
    seq_count = hidden_in.shape[0]
    route_count = route_ids.shape[1]
    local_experts = expert_gate.shape[0]
    experts = local_experts * lax.axis_size("ep")
    capacity = min(seq_count, max(2, 2 * seq_count * route_count // experts))
    flat_ids = route_ids.reshape(-1)
    expert_iota = jnp.arange(experts, dtype=jnp.int32)
    onehot = (flat_ids[:, None] == expert_iota[None, :]).astype(jnp.int32)
    earlier = jnp.cumsum(onehot, axis=0) - onehot
    slot_index = flat_ids * capacity + jnp.sum(earlier * onehot, axis=1)
    slot_iota = jnp.arange(experts * capacity, dtype=jnp.int32)
    placement = (slot_index[:, None] == slot_iota[None, :]).astype(jnp.bfloat16)
    repeated = jnp.repeat(normed_part, route_count, axis=0)
    outgoing = jnp.einsum("ke,kd->ed", placement, repeated, preferred_element_type=jnp.float32)
    full_rows = lax.all_gather(
        lax.all_to_all(
            outgoing.astype(jnp.bfloat16).reshape(experts, capacity, normed_part.shape[1]),
            "ep",
            split_axis=0,
            concat_axis=0,
            tiled=True,
        ),
        "tp",
        axis=2,
        tiled=True,
    )
    senders = full_rows.shape[0] // local_experts
    grouped = full_rows.reshape(senders, local_experts, full_rows.shape[1], full_rows.shape[2])
    gate_act = jnp.einsum(
        "secd,edf->secf", grouped, expert_gate, preferred_element_type=jnp.float32
    )
    up_act = jnp.einsum("secd,edf->secf", grouped, expert_up, preferred_element_type=jnp.float32)
    hidden = (jax.nn.silu(gate_act) * up_act).astype(jnp.bfloat16)
    partial_value = jnp.einsum(
        "secf,efd->secd", hidden, expert_down, preferred_element_type=jnp.float32
    )
    partial_value = partial_value.astype(jnp.bfloat16)
    summed = lax.psum_scatter(
        partial_value.astype(jnp.float32).astype(jnp.bfloat16),
        "tp",
        scatter_dimension=3,
        tiled=True,
    )
    summed = summed.reshape(senders * local_experts, summed.shape[2], summed.shape[3])
    returned = lax.all_to_all(summed, "ep", split_axis=0, concat_axis=0, tiled=True)
    flat_back = returned.reshape(experts * capacity, returned.shape[2])
    picked = jnp.take(flat_back, slot_index, axis=0)
    picked = picked.astype(jnp.float32).reshape(seq_count, route_count, slice_width)
    route_weight = route_scores / jnp.sum(route_scores, axis=1, keepdims=True)
    expert_mix = jnp.sum(picked * route_weight[:, :, None], axis=1)
    hidden_out = (residual.astype(jnp.float32) + expert_mix).astype(jnp.bfloat16)
    return (hidden_out, new_keys, new_values)


def layer_kernel(
    sizes,
    hid_ref,
    attn_gain_ref,
    bias_ref,
    lengths_ref,
    gain_ref,
    ids_ref,
    scores_ref,
    wq_hbm,
    wk_hbm,
    wv_hbm,
    key_hbm,
    value_hbm,
    wo_hbm,
    gate_hbm,
    up_hbm,
    down_hbm,
    out_ref,
    new_key_ref,
    new_value_ref,
    w_in,
    key_c,
    value_c,
    wo_full,
    gate_w,
    up_w,
    down_w,
    hid_both,
    normed_in,
    logits,
    spans,
    stick,
    att_both,
    resid,
    rows,
    own,
    for_sib,
    from_sib,
    stage_a,
    recv_a,
    stage_b,
    recv_b,
    stage_c,
    recv_c,
    stage_d,
    recv_d,
    load_sem,
    pair_send,
    pair_recv,
    z_send,
    z_recv,
    two_send,
    two_recv,
    three_send,
    three_recv,
    sib_send,
    sib_recv,
    red_send,
    red_recv,
    a_send,
    a_recv,
    b_send,
    b_recv,
):
    tokens, padded, zs, width, half, experts, heads = sizes
    live = tokens + -tokens % 8
    quarter = half // 2
    columns_in = heads * HEAD_DIM
    ep = lax.axis_index("ep")
    y = lax.axis_index("tp")
    c = lax.rem(ep, 2)
    x = lax.rem(ep // 2, 2)
    z = ep // 4

    def device(zi, xi, ci, yi):
        return {"ep": zi * 4 + xi * 2 + ci, "tp": yi}

    sibling = device(z, x, 1 - c, y)
    across_y = device(z, x, c, 1 - y)
    across_x = device(z, 1 - x, c, y)
    axis_two = device(z, x + (1 - c) * (1 - 2 * x), c, y + c * (1 - 2 * y))
    axis_three = device(z, x + c * (1 - 2 * x), c, y + (1 - c) * (1 - 2 * y))

    sources = [
        (wq_hbm, w_in.at[0]),
        (wk_hbm, w_in.at[1]),
        (wv_hbm, w_in.at[2]),
        (key_hbm, key_c),
        (value_hbm, value_c),
        (wo_hbm, wo_full.at[y]),
        (gate_hbm.at[0], gate_w),
        (up_hbm.at[0], up_w),
        (down_hbm.at[0], down_w),
    ]
    loads = [
        pltpu.make_async_copy(src, dst, load_sem.at[i]) for i, (src, dst) in enumerate(sources)
    ]
    for load in loads:
        load.start()

    barrier = pltpu.get_barrier_semaphore()
    partners = [sibling, across_y, across_x] + [
        device(lax.rem(z + d, zs), x, c, y) for d in range(1, zs)
    ]
    for partner in partners:
        pl.semaphore_signal(
            barrier, inc=1, device_id=partner, device_id_type=pl.DeviceIdType.MESH
        )
    pl.semaphore_wait(barrier, len(partners))

    pending = []

    def send(src, dst, send_sem, recv_sem, target):
        copy = pltpu.make_async_remote_copy(
            src_ref=src,
            dst_ref=dst,
            send_sem=send_sem,
            recv_sem=recv_sem,
            device_id=target,
            device_id_type=pl.DeviceIdType.MESH,
        )
        copy.start()
        pending.append(copy)
        return copy

    give = send(hid_ref, hid_both.at[y], pair_send.at[0], pair_recv.at[0], across_y)
    wo_rows = columns_in // 2
    wo_part = pl.ds(pl.multiple_of(c * wo_rows, wo_rows), wo_rows)
    give_wo = send(
        wo_hbm.at[wo_part], wo_full.at[y, wo_part], pair_send.at[1], pair_recv.at[1], across_y
    )
    hid_both[y] = hid_ref[...]
    normed_in[...] = jnp.zeros_like(normed_in)

    scores = scores_ref[...]
    route_weight = scores / jnp.sum(scores, axis=1, keepdims=True)
    high = route_weight.astype(jnp.bfloat16).astype(jnp.float32)
    low = route_weight - high
    ids = ids_ref[...]
    extra = rows.shape[-1] - half
    lane = lax.broadcasted_iota(jnp.int32, (tokens, extra), 1)
    coded = jnp.zeros((tokens, extra), jnp.float32)
    for k in range(ids.shape[1]):
        name = ids[:, k : k + 1]
        coded += jnp.where(lane == name, high[:, k : k + 1], 0.0)
        coded += jnp.where(lane == name + experts, low[:, k : k + 1], 0.0)
    rows[y, x, z, c, :tokens, half:] = coded.astype(jnp.bfloat16)

    give.wait_recv()
    left = hid_both[0].astype(jnp.float32)
    right = hid_both[1].astype(jnp.float32)
    square = jnp.sum(left * left, axis=1, keepdims=True) + jnp.sum(
        right * right, axis=1, keepdims=True
    )
    inverse = lax.rsqrt(square / width + norm_eps)
    normed_in[:tokens, :half] = (left * inverse * attn_gain_ref[:, :half]).astype(jnp.bfloat16)
    normed_in[:tokens, half:] = (right * inverse * attn_gain_ref[:, half:]).astype(jnp.bfloat16)
    for load in loads[:3]:
        load.wait()
    across = (((1,), (1,)), ((), ()))
    q_cols = lax.dot_general(
        w_in[0], normed_in[...], across, preferred_element_type=jnp.float32
    )
    q_cols = q_cols.astype(jnp.bfloat16).astype(jnp.float32)
    for i, ref in ((1, new_key_ref), (2, new_value_ref)):
        made = lax.dot_general(
            normed_in[...], w_in[i], across, preferred_element_type=jnp.float32
        )
        ref[...] = made[:tokens].astype(jnp.bfloat16)

    span = key_c.shape[2]
    q_lane = lax.broadcasted_iota(jnp.int32, q_cols.shape, 1)
    loads[3].wait()

    def score(t, carry):
        column = jnp.sum(jnp.where(q_lane == t, q_cols, 0.0), axis=1, keepdims=True)
        scaled = key_c[t].astype(jnp.float32) * column
        for h in range(heads):
            summed_h = jnp.sum(scaled[h * HEAD_DIM : (h + 1) * HEAD_DIM], axis=0, keepdims=True)
            logits[h, pl.ds(t, 1), :] = summed_h * HEAD_DIM ** (-0.5) + bias_ref[h]
        spans[pl.ds(t, 1), :] = jnp.full((1, span), lengths_ref[t], jnp.int32)
        return carry

    lax.fori_loop(0, tokens, score, 0, unroll=2)
    row = lax.broadcasted_iota(jnp.int32, (span, span), 0)
    col = lax.broadcasted_iota(jnp.int32, (span, span), 1)
    later = (row > col).astype(jnp.float32).astype(jnp.bfloat16)
    position = lax.broadcasted_iota(jnp.int32, (padded, span), 1)
    visible = position < spans[...]
    for h in range(heads):
        logit = logits[h]
        soft = jnp.log1p(jnp.exp(-jnp.abs(logit)))
        log_keep = jnp.where(visible, -jnp.maximum(logit, 0.0) - soft, 0.0)
        total, rest = 0.0, log_keep
        for _ in range(3):
            term = rest.astype(jnp.bfloat16)
            rest = rest - term.astype(jnp.float32)
            total = total + jnp.dot(term, later, preferred_element_type=jnp.float32)
        value = jnp.where(visible, jnp.exp(jnp.minimum(logit, 0.0) - soft + total), 0.0)
        stick[h] = value.astype(jnp.bfloat16).astype(jnp.float32)
    loads[4].wait()
    att_lane = lax.broadcasted_iota(jnp.int32, (columns_in, 128), 1)

    def attend(t, gathered):
        parts = []
        for h in range(heads):
            part = value_c[t, h * HEAD_DIM : (h + 1) * HEAD_DIM].astype(jnp.float32)
            parts.append(
                jnp.sum(part * stick[h, pl.ds(t, 1), :], axis=1, keepdims=True)
            )
        column = jnp.concatenate(parts, axis=0)
        return jnp.where(att_lane == t, column, gathered)

    gathered = lax.fori_loop(
        0, tokens, attend, jnp.zeros((columns_in, 128), jnp.float32), unroll=2
    )
    att_both[y] = gathered.T[:padded].astype(jnp.bfloat16)
    give_att = send(
        att_both.at[y], att_both.at[y], pair_send.at[2], pair_recv.at[2], across_y
    )
    give_wo.wait_recv()
    came = wo_full.at[1 - y, wo_part]
    share_wo = send(came, came, pair_send.at[3], pair_recv.at[3], sibling)
    loads[5].wait()
    share_wo.wait_recv()
    give_att.wait_recv()
    mixer = jnp.dot(att_both[0], wo_full[0], preferred_element_type=jnp.float32)
    mixer += jnp.dot(att_both[1], wo_full[1], preferred_element_type=jnp.float32)
    left = (left + mixer[:tokens, :half]).astype(jnp.bfloat16).astype(jnp.float32)
    right = (right + mixer[:tokens, half:]).astype(jnp.bfloat16).astype(jnp.float32)
    square = jnp.sum(left * left, axis=1, keepdims=True) + jnp.sum(
        right * right, axis=1, keepdims=True
    )
    inverse = lax.rsqrt(square / width + norm_eps)
    mine = pl.ds(pl.multiple_of(y * half, half), half)
    values = jnp.where(y == 0, left, right)
    resid[...] = values
    rows[y, x, z, c, :tokens, :half] = (values * inverse * gain_ref[:, mine]).astype(
        jnp.bfloat16
    )

    def block(yi, xi, zi):
        return rows.at[yi, xi, zi, c, pl.ds(0, live), :]

    def share(where, slot, send_sem, recv_sem, target):
        ref = block(*where)
        return send(ref, ref, send_sem.at[slot], recv_sem.at[slot], target)

    from_z, from_two, from_three, from_core = [], [], [], []
    me = (y, x, z)
    for d in range(1, zs):
        from_z.append(
            share(me, d - 1, z_send, z_recv, device(lax.rem(z + d, zs), x, c, y))
        )
    for d in range(zs):
        if d > 0:
            from_z[d - 1].wait_recv()
        where = (y, x, lax.rem(z - d + zs, zs))
        from_two.append(share(where, d, two_send, two_recv, axis_two))
        from_three.append(share(where, d, three_send, three_recv, axis_three))
        from_core.append(share(where, d, sib_send, sib_recv, sibling))
    x_two, y_two = x + (1 - c) * (1 - 2 * x), y + c * (1 - 2 * y)
    for d in range(zs):
        from_two[d].wait_recv()
        where = (y_two, x_two, lax.rem(z - d + zs, zs))
        from_three.append(share(where, zs + d, three_send, three_recv, axis_three))
        from_core.append(share(where, zs + d, sib_send, sib_recv, sibling))
    x_three, y_three = x + c * (1 - 2 * x), y + (1 - c) * (1 - 2 * y)
    for d in range(2 * zs):
        from_three[d].wait_recv()
        zi = lax.rem(z - d + 2 * zs, zs)
        where = (y_three, x_three, zi) if d < zs else (1 - y, 1 - x, zi)
        from_core.append(share(where, 2 * zs + d, sib_send, sib_recv, sibling))
    for copy in from_core:
        copy.wait_recv()
    for load in loads[6:]:
        load.wait()

    count = 4 * zs * padded
    gate_act, up_act = 0.0, 0.0
    for yi in range(2):
        taken = rows[yi, :, :, :, :, :half].reshape(count, half)
        depth = slice(yi * half, (yi + 1) * half)
        gate_act += jnp.dot(taken, gate_w[depth], preferred_element_type=jnp.float32)
        up_act += jnp.dot(taken, up_w[depth], preferred_element_type=jnp.float32)
    hidden = (jax.nn.silu(gate_act) * up_act).astype(jnp.bfloat16)
    coded = rows[0, :, :, :, :, half:].reshape(count, -1).astype(jnp.float32)
    lane = lax.broadcasted_iota(jnp.int32, coded.shape, 1)
    named = (lane == ep) | (lane == ep + experts)
    weight = jnp.sum(jnp.where(named, coded, 0.0), axis=1, keepdims=True)

    def piece(yi, ci):
        columns = pl.ds(pl.multiple_of(yi * half + ci * quarter, quarter), quarter)
        result = jnp.dot(hidden, down_w[:, columns], preferred_element_type=jnp.float32)
        return (result * weight).reshape(2, zs, 2, padded, quarter)

    halves = []
    some = (slice(None), slice(None), slice(None), pl.ds(0, live), slice(None))
    for yi in range(2):
        for_sib[yi] = piece(yi, 1 - c).astype(jnp.bfloat16)
        halves.append(
            send(
                for_sib.at[(yi,) + some],
                from_sib.at[(yi,) + some],
                red_send.at[yi],
                red_recv.at[yi],
                sibling,
            )
        )
    for yi in range(2):
        own[yi] = piece(yi, c)
    for copy in halves:
        copy.wait_recv()

    one = y + c * (x - y)
    two = x + c * (y - x)

    def summed(fi, si, zi):
        yi, xi = fi + c * (si - fi), si + c * (fi - si)
        return own[yi, xi, zi] + from_sib[yi, xi, zi].astype(jnp.float32)

    order = [lax.rem(z + d, zs) for d in list(range(1, zs)) + [0]]
    cut = (slice(None), pl.ds(0, live), slice(None))
    to_first, to_second, along_z = [], [], []
    for j, si in enumerate((1 - two, two)):
        for i, zi in enumerate(order):
            stage_a[si, zi] = summed(1 - one, si, zi).astype(jnp.bfloat16)
            at = (si, zi) + cut
            slot = j * zs + i
            to_first.append(
                send(stage_a.at[at], recv_a.at[at], a_send.at[slot], a_recv.at[slot], axis_three)
            )
    for i, zi in enumerate(order):
        to_first[i].wait_recv()
        stage_b[zi] = (
            summed(one, 1 - two, zi) + recv_a[1 - two, zi].astype(jnp.float32)
        ).astype(jnp.bfloat16)
        at = (zi,) + cut
        to_second.append(
            send(stage_b.at[at], recv_b.at[at], b_send.at[i], b_recv.at[i], axis_two)
        )
    for i, zi in enumerate(order):
        to_first[zs + i].wait_recv()
        to_second[i].wait_recv()
        kept = (
            summed(one, two, zi)
            + recv_a[two, zi].astype(jnp.float32)
            + recv_b[zi].astype(jnp.float32)
        )
        if i < zs - 1:
            stage_c[zi] = kept.astype(jnp.bfloat16)
            along_z.append(
                send(
                    stage_c.at[(zi,) + cut],
                    recv_c.at[(i,) + cut],
                    red_send.at[3 + i],
                    red_recv.at[3 + i],
                    device(zi, x, c, y),
                )
            )
    total = kept
    for i in range(zs - 1):
        along_z[i].wait_recv()
        total = total + recv_c[i].astype(jnp.float32)
    stage_d[...] = total
    last = send(stage_d.at[1 - c], recv_d, red_send.at[2], red_recv.at[2], sibling)
    near = pl.ds(pl.multiple_of(c * quarter, quarter), quarter)
    far = pl.ds(pl.multiple_of((1 - c) * quarter, quarter), quarter)
    out_ref[:, near] = (resid[:, near] + stage_d[c, :tokens]).astype(out_ref.dtype)
    last.wait_recv()
    out_ref[:, far] = (resid[:, far] + recv_d[:tokens]).astype(out_ref.dtype)
    for copy in pending:
        copy.wait_send()


def dense_shards(
    hidden_in,
    attn_gain,
    w_query,
    w_key,
    w_value,
    break_bias,
    key_cache,
    value_cache,
    lengths,
    w_out,
    ffn_gain,
    route_ids,
    route_scores,
    expert_gate,
    expert_up,
    expert_down,
):
    tokens, half = hidden_in.shape
    padded = tokens + -tokens % 16
    width = 2 * half
    experts = lax.axis_size("ep")
    heads = break_bias.shape[0]
    zs = experts // 4
    extra = 2 * experts + -2 * experts % 128
    blocks = (2, zs, 2, padded, half // 2)
    bf16, f32 = jnp.bfloat16, jnp.float32
    vmem = pl.BlockSpec(memory_space=pltpu.VMEM)
    smem = pl.BlockSpec(memory_space=pltpu.SMEM)
    hbm = pl.BlockSpec(memory_space=pl.ANY)
    dma = pltpu.SemaphoreType.DMA
    columns_in, span = key_cache.shape[1:]
    sizes = (tokens, padded, zs, width, half, experts, heads)
    new_shape = jax.ShapeDtypeStruct((tokens, columns_in), bf16)
    pairs = [4, zs - 1, zs, 2 * zs, 4 * zs, 3 + zs, 2 * zs, zs]
    return pl.pallas_call(
        functools.partial(layer_kernel, sizes),
        out_shape=(jax.ShapeDtypeStruct((tokens, half), bf16), new_shape, new_shape),
        in_specs=[vmem, vmem, smem, smem, vmem, vmem, vmem] + [hbm] * 9,
        out_specs=(vmem, vmem, vmem),
        scratch_shapes=[
            pltpu.VMEM((3,) + w_query.shape, bf16),
            pltpu.VMEM(key_cache.shape, bf16),
            pltpu.VMEM(value_cache.shape, bf16),
            pltpu.VMEM((2,) + w_out.shape, bf16),
            pltpu.VMEM(expert_gate.shape[1:], bf16),
            pltpu.VMEM(expert_up.shape[1:], bf16),
            pltpu.VMEM(expert_down.shape[1:], bf16),
            pltpu.VMEM((2, tokens, half), bf16),
            pltpu.VMEM((padded, width), bf16),
            pltpu.VMEM((heads, padded, span), f32),
            pltpu.VMEM((padded, span), jnp.int32),
            pltpu.VMEM((heads, padded, span), f32),
            pltpu.VMEM((2, padded, columns_in), bf16),
            pltpu.VMEM((tokens, half), f32),
            pltpu.VMEM((2, 2, zs, 2, padded, half + extra), bf16),
            pltpu.VMEM((2,) + blocks, f32),
            pltpu.VMEM((2,) + blocks, bf16),
            pltpu.VMEM((2,) + blocks, bf16),
            pltpu.VMEM(blocks, bf16),
            pltpu.VMEM(blocks, bf16),
            pltpu.VMEM(blocks[1:], bf16),
            pltpu.VMEM(blocks[1:], bf16),
            pltpu.VMEM(blocks[1:], bf16),
            pltpu.VMEM((zs - 1,) + blocks[2:], bf16),
            pltpu.VMEM(blocks[2:], f32),
            pltpu.VMEM(blocks[3:], f32),
            dma((9,)),
        ]
        + [dma((count,)) for count in pairs for _ in range(2)],
        compiler_params=pltpu.CompilerParams(
            collective_id=0, has_side_effects=True, vmem_limit_bytes=60 * 1024 * 1024
        ),
    )(
        hidden_in,
        attn_gain[None, :],
        break_bias,
        lengths,
        ffn_gain[None, :],
        route_ids,
        route_scores,
        w_query,
        w_key,
        w_value,
        key_cache,
        value_cache,
        w_out,
        expert_gate,
        expert_up,
        expert_down,
    )


def solution(mesh):
    ep_size, tp_size = mesh.shape["ep"], mesh.shape["tp"]
    fits = tp_size == 2 and ep_size % 4 == 0 and 8 <= ep_size <= 16
    body = dense_shards if fits else shards
    return jax.shard_map(
        body,
        mesh=mesh,
        in_specs=(
            P("ep", "tp"),
            P(),
            P("tp", None),
            P("tp", None),
            P("tp", None),
            P("tp"),
            P("ep", "tp", None),
            P("ep", "tp", None),
            P("ep"),
            P("tp", None),
            P(),
            P("ep", None),
            P("ep", None),
            P("ep", None, "tp"),
            P("ep", None, "tp"),
            P("ep", "tp", None),
        ),
        out_specs=(P("ep", "tp"), P("ep", "tp"), P("ep", "tp")),
        check_vma=False,
    )
```

```python
import functools

import jax
import jax.numpy as jnp
from jax import lax
from jax.experimental import pallas as pl
from jax.experimental.pallas import tpu as pltpu
from jax.sharding import PartitionSpec as P

HEAD_DIM = 64


norm_eps = 1e-06


def rms_norm(row_values, norm_gain):
    values = row_values.astype(jnp.float32)
    inverse_rms = lax.rsqrt(jnp.mean(values * values, axis=-1, keepdims=True) + norm_eps)
    return (values * inverse_rms * norm_gain).astype(jnp.bfloat16)


def project_rows(normed, weight):
    return lax.dot_general(
        normed, weight, (((1,), (1,)), ((), ())), preferred_element_type=jnp.float32
    ).astype(jnp.bfloat16)


def stick_breaking(queries, key_block, value_block, lengths, break_bias):
    head_count = break_bias.shape[0]
    q_heads = queries.reshape(queries.shape[0], head_count, HEAD_DIM)
    k_heads = key_block.reshape(key_block.shape[0], head_count, HEAD_DIM, key_block.shape[2])
    v_heads = value_block.reshape(value_block.shape[0], head_count, HEAD_DIM, value_block.shape[2])
    logit = jnp.einsum("shd,shdl->shl", q_heads, k_heads, preferred_element_type=jnp.float32)
    logit = logit * HEAD_DIM ** (-0.5) + break_bias[None, :, None]
    position = jnp.arange(key_block.shape[2], dtype=jnp.int32)
    visible = (position[None, :] < lengths[:, None])[:, None, :]
    log_keep = jnp.where(visible, jax.nn.log_sigmoid(-logit), 0.0)
    later_sum = lax.cumsum(log_keep, axis=2, reverse=True) - log_keep
    stick = jnp.where(visible, jnp.exp(jax.nn.log_sigmoid(logit) + later_sum), 0.0).astype(
        jnp.bfloat16
    )
    attended = jnp.einsum("shl,shdl->shd", stick, v_heads, preferred_element_type=jnp.float32)
    return attended.reshape(queries.shape[0], -1).astype(jnp.bfloat16)


def shards(
    hidden_in,
    attn_gain,
    w_query,
    w_key,
    w_value,
    break_bias,
    key_cache,
    value_cache,
    lengths,
    w_out,
    ffn_gain,
    route_ids,
    route_scores,
    expert_gate,
    expert_up,
    expert_down,
):
    gathered = lax.all_gather(hidden_in, "tp", axis=1, tiled=True)
    full_width = gathered.shape[1]
    slice_width = hidden_in.shape[1]
    offset = lax.axis_index("tp") * slice_width
    normed_attn = rms_norm(gathered, attn_gain)
    queries = project_rows(normed_attn, w_query)
    new_keys = project_rows(normed_attn, w_key)
    new_values = project_rows(normed_attn, w_value)
    attended = stick_breaking(queries, key_cache, value_cache, lengths, break_bias)
    partial_out = jnp.dot(attended, w_out, preferred_element_type=jnp.float32)
    mixer_part = lax.psum_scatter(partial_out, "tp", scatter_dimension=1, tiled=True)
    residual = (hidden_in.astype(jnp.float32) + mixer_part).astype(jnp.bfloat16)
    resid_values = residual.astype(jnp.float32)
    square_total = lax.psum(jnp.sum(resid_values * resid_values, axis=1), "tp")
    inverse_rms = lax.rsqrt(square_total / full_width + norm_eps)
    gain_part = lax.dynamic_slice_in_dim(ffn_gain, offset, slice_width)
    normed_part = (resid_values * inverse_rms[:, None] * gain_part[None, :]).astype(jnp.bfloat16)
    seq_count = hidden_in.shape[0]
    route_count = route_ids.shape[1]
    local_experts = expert_gate.shape[0]
    experts = local_experts * lax.axis_size("ep")
    capacity = min(seq_count, max(2, 2 * seq_count * route_count // experts))
    flat_ids = route_ids.reshape(-1)
    expert_iota = jnp.arange(experts, dtype=jnp.int32)
    onehot = (flat_ids[:, None] == expert_iota[None, :]).astype(jnp.int32)
    earlier = jnp.cumsum(onehot, axis=0) - onehot
    slot_index = flat_ids * capacity + jnp.sum(earlier * onehot, axis=1)
    slot_iota = jnp.arange(experts * capacity, dtype=jnp.int32)
    placement = (slot_index[:, None] == slot_iota[None, :]).astype(jnp.bfloat16)
    repeated = jnp.repeat(normed_part, route_count, axis=0)
    outgoing = jnp.einsum("ke,kd->ed", placement, repeated, preferred_element_type=jnp.float32)
    full_rows = lax.all_gather(
        lax.all_to_all(
            outgoing.astype(jnp.bfloat16).reshape(experts, capacity, normed_part.shape[1]),
            "ep",
            split_axis=0,
            concat_axis=0,
            tiled=True,
        ),
        "tp",
        axis=2,
        tiled=True,
    )
    senders = full_rows.shape[0] // local_experts
    grouped = full_rows.reshape(senders, local_experts, full_rows.shape[1], full_rows.shape[2])
    gate_act = jnp.einsum(
        "secd,edf->secf", grouped, expert_gate, preferred_element_type=jnp.float32
    )
    up_act = jnp.einsum("secd,edf->secf", grouped, expert_up, preferred_element_type=jnp.float32)
    hidden = (jax.nn.silu(gate_act) * up_act).astype(jnp.bfloat16)
    partial_value = jnp.einsum(
        "secf,efd->secd", hidden, expert_down, preferred_element_type=jnp.float32
    )
    partial_value = partial_value.astype(jnp.bfloat16)
    summed = lax.psum_scatter(
        partial_value.astype(jnp.float32).astype(jnp.bfloat16),
        "tp",
        scatter_dimension=3,
        tiled=True,
    )
    summed = summed.reshape(senders * local_experts, summed.shape[2], summed.shape[3])
    returned = lax.all_to_all(summed, "ep", split_axis=0, concat_axis=0, tiled=True)
    flat_back = returned.reshape(experts * capacity, returned.shape[2])
    picked = jnp.take(flat_back, slot_index, axis=0)
    picked = picked.astype(jnp.float32).reshape(seq_count, route_count, slice_width)
    route_weight = route_scores / jnp.sum(route_scores, axis=1, keepdims=True)
    expert_mix = jnp.sum(picked * route_weight[:, :, None], axis=1)
    hidden_out = (residual.astype(jnp.float32) + expert_mix).astype(jnp.bfloat16)
    return (hidden_out, new_keys, new_values)


def hand_on(*refs):
    for source, target in zip(refs[:3], refs[3:]):
        target[...] = source[...]


def layer_kernel(
    sizes,
    hid_ref,
    attn_gain_ref,
    bias_ref,
    lengths_ref,
    gain_ref,
    ids_ref,
    scores_ref,
    wq_hbm,
    wk_hbm,
    wv_hbm,
    key_hbm,
    value_hbm,
    wo_hbm,
    gate_hbm,
    up_hbm,
    down_hbm,
    out_ref,
    new_key_ref,
    new_value_ref,
    w_in,
    key_c,
    value_c,
    wo_full,
    gate_w,
    up_w,
    down_w,
    hid_both,
    normed_in,
    logits,
    spans,
    stick,
    turn,
    att_both,
    resid,
    rows,
    own,
    for_sib,
    from_sib,
    stage_a,
    recv_a,
    stage_b,
    recv_b,
    stage_c,
    recv_c,
    stage_d,
    recv_d,
    load_sem,
    pair_send,
    pair_recv,
    z_send,
    z_recv,
    two_send,
    two_recv,
    three_send,
    three_recv,
    sib_send,
    sib_recv,
    red_send,
    red_recv,
    a_send,
    a_recv,
    b_send,
    b_recv,
):
    tokens, padded, zs, width, half, experts, heads = sizes
    live = tokens + -tokens % 8
    quarter = half // 2
    columns_in = heads * HEAD_DIM
    ep = lax.axis_index("ep")
    y = lax.axis_index("tp")
    c = lax.rem(ep, 2)
    x = lax.rem(ep // 2, 2)
    z = ep // 4

    def device(zi, xi, ci, yi):
        return {"ep": zi * 4 + xi * 2 + ci, "tp": yi}

    sibling = device(z, x, 1 - c, y)
    across_y = device(z, x, c, 1 - y)
    across_x = device(z, 1 - x, c, y)
    axis_two = device(z, x + (1 - c) * (1 - 2 * x), c, y + c * (1 - 2 * y))
    axis_three = device(z, x + c * (1 - 2 * x), c, y + (1 - c) * (1 - 2 * y))

    sources = [
        (wq_hbm, w_in.at[0]),
        (wk_hbm, w_in.at[1]),
        (wv_hbm, w_in.at[2]),
        (key_hbm, key_c),
        (value_hbm, value_c),
        (wo_hbm, wo_full.at[y]),
        (gate_hbm.at[0], gate_w),
        (up_hbm.at[0], up_w),
        (down_hbm.at[0], down_w),
    ]
    loads = [
        pltpu.make_async_copy(src, dst, load_sem.at[i]) for i, (src, dst) in enumerate(sources)
    ]
    for load in loads[:6]:
        load.start()

    barrier = pltpu.get_barrier_semaphore()
    partners = [sibling, across_y, across_x] + [
        device(lax.rem(z + d, zs), x, c, y) for d in range(1, zs)
    ]
    for partner in partners:
        pl.semaphore_signal(
            barrier, inc=1, device_id=partner, device_id_type=pl.DeviceIdType.MESH
        )
    pl.semaphore_wait(barrier, len(partners))

    pending = []

    def send(src, dst, send_sem, recv_sem, target):
        copy = pltpu.make_async_remote_copy(
            src_ref=src,
            dst_ref=dst,
            send_sem=send_sem,
            recv_sem=recv_sem,
            device_id=target,
            device_id_type=pl.DeviceIdType.MESH,
        )
        copy.start()
        pending.append(copy)
        return copy

    give = send(hid_ref, hid_both.at[y], pair_send.at[0], pair_recv.at[0], across_y)
    wo_rows = columns_in // 2
    wo_part = pl.ds(pl.multiple_of(c * wo_rows, wo_rows), wo_rows)
    give_wo = send(
        wo_hbm.at[wo_part], wo_full.at[y, wo_part], pair_send.at[1], pair_recv.at[1], across_y
    )
    hid_both[y] = hid_ref[...]
    normed_in[...] = jnp.zeros_like(normed_in)

    scores = scores_ref[...]
    route_weight = scores / jnp.sum(scores, axis=0, keepdims=True)
    high = route_weight.astype(jnp.bfloat16).astype(jnp.float32)
    low = route_weight - high
    ids = ids_ref[...]
    extra = rows.shape[-1] - half
    place = lax.broadcasted_iota(jnp.int32, (extra, tokens), 0)
    coded = jnp.zeros((extra, tokens), jnp.float32)
    for k in range(ids.shape[0]):
        name = ids[k : k + 1]
        coded += jnp.where(place == name, high[k : k + 1], 0.0)
        coded += jnp.where(place == name + experts, low[k : k + 1], 0.0)
    turn[...] = jnp.zeros_like(turn)
    turn[:, :tokens] = coded
    rows[y, x, z, c, :tokens, half:] = turn[...].T[:tokens].astype(jnp.bfloat16)

    give.wait_recv()
    left = hid_both[0].astype(jnp.float32)
    right = hid_both[1].astype(jnp.float32)
    square = jnp.sum(left * left, axis=1, keepdims=True) + jnp.sum(
        right * right, axis=1, keepdims=True
    )
    inverse = lax.rsqrt(square / width + norm_eps)
    normed_in[:tokens, :half] = (left * inverse * attn_gain_ref[:, :half]).astype(jnp.bfloat16)
    normed_in[:tokens, half:] = (right * inverse * attn_gain_ref[:, half:]).astype(jnp.bfloat16)
    for load in loads[:3]:
        load.wait()
    across = (((1,), (1,)), ((), ()))
    q_cols = lax.dot_general(
        w_in[0], normed_in[...], across, preferred_element_type=jnp.float32
    )
    q_cols = q_cols.astype(jnp.bfloat16).astype(jnp.float32)
    for i, ref in ((1, new_key_ref), (2, new_value_ref)):
        made = lax.dot_general(
            normed_in[...], w_in[i], across, preferred_element_type=jnp.float32
        )
        ref[...] = made[:tokens].astype(jnp.bfloat16)

    span = key_c.shape[2]
    q_lane = lax.broadcasted_iota(jnp.int32, q_cols.shape, 1)
    loads[3].wait()
    for load in loads[6:]:
        load.start()

    def score(t, carry):
        column = jnp.sum(jnp.where(q_lane == t, q_cols, 0.0), axis=1, keepdims=True)
        scaled = key_c[t].astype(jnp.float32) * column
        for h in range(heads):
            summed_h = jnp.sum(scaled[h * HEAD_DIM : (h + 1) * HEAD_DIM], axis=0, keepdims=True)
            logits[h, pl.ds(t, 1), :] = summed_h * HEAD_DIM ** (-0.5) + bias_ref[h]
        spans[pl.ds(t, 1), :] = jnp.full((1, span), lengths_ref[t], jnp.int32)
        return carry

    lax.fori_loop(0, tokens, score, 0, unroll=5)
    row = lax.broadcasted_iota(jnp.int32, (span, span), 0)
    col = lax.broadcasted_iota(jnp.int32, (span, span), 1)
    later = (row > col).astype(jnp.float32).astype(jnp.bfloat16)
    position = lax.broadcasted_iota(jnp.int32, (padded, span), 1)
    visible = position < spans[...]
    for h in range(heads):
        logit = logits[h]
        soft = jnp.log1p(jnp.exp(-jnp.abs(logit)))
        log_keep = jnp.where(visible, -jnp.maximum(logit, 0.0) - soft, 0.0)
        total, rest = 0.0, log_keep
        for _ in range(3):
            term = rest.astype(jnp.bfloat16)
            rest = rest - term.astype(jnp.float32)
            total = total + jnp.dot(term, later, preferred_element_type=jnp.float32)
        value = jnp.where(visible, jnp.exp(jnp.minimum(logit, 0.0) - soft + total), 0.0)
        stick[h] = value.astype(jnp.bfloat16).astype(jnp.float32)
    loads[4].wait()
    att_lane = lax.broadcasted_iota(jnp.int32, (columns_in, 128), 1)

    def attend(t, gathered):
        parts = []
        for h in range(heads):
            part = value_c[t, h * HEAD_DIM : (h + 1) * HEAD_DIM].astype(jnp.float32)
            parts.append(
                jnp.sum(part * stick[h, pl.ds(t, 1), :], axis=1, keepdims=True)
            )
        column = jnp.concatenate(parts, axis=0)
        return jnp.where(att_lane == t, column, gathered)

    gathered = lax.fori_loop(
        0, tokens, attend, jnp.zeros((columns_in, 128), jnp.float32), unroll=5
    )
    att_both[y] = gathered.T[:padded].astype(jnp.bfloat16)
    give_att = send(
        att_both.at[y], att_both.at[y], pair_send.at[2], pair_recv.at[2], across_y
    )
    give_wo.wait_recv()
    came = wo_full.at[1 - y, wo_part]
    share_wo = send(came, came, pair_send.at[3], pair_recv.at[3], sibling)
    loads[5].wait()
    share_wo.wait_recv()
    give_att.wait_recv()
    mixer = jnp.dot(att_both[0], wo_full[0], preferred_element_type=jnp.float32)
    mixer += jnp.dot(att_both[1], wo_full[1], preferred_element_type=jnp.float32)
    left = (left + mixer[:tokens, :half]).astype(jnp.bfloat16).astype(jnp.float32)
    right = (right + mixer[:tokens, half:]).astype(jnp.bfloat16).astype(jnp.float32)
    square = jnp.sum(left * left, axis=1, keepdims=True) + jnp.sum(
        right * right, axis=1, keepdims=True
    )
    inverse = lax.rsqrt(square / width + norm_eps)
    mine = pl.ds(pl.multiple_of(y * half, half), half)
    values = jnp.where(y == 0, left, right)
    resid[...] = values
    rows[y, x, z, c, :tokens, :half] = (values * inverse * gain_ref[:, mine]).astype(
        jnp.bfloat16
    )

    def block(yi, xi, zi):
        return rows.at[yi, xi, zi, c, pl.ds(0, live), :]

    def share(where, slot, send_sem, recv_sem, target):
        ref = block(*where)
        return send(ref, ref, send_sem.at[slot], recv_sem.at[slot], target)

    from_z, from_two, from_three, from_core = [], [], [], []
    me = (y, x, z)
    for d in range(1, zs):
        from_z.append(
            share(me, d - 1, z_send, z_recv, device(lax.rem(z + d, zs), x, c, y))
        )
    for d in range(zs):
        if d > 0:
            from_z[d - 1].wait_recv()
        where = (y, x, lax.rem(z - d + zs, zs))
        from_two.append(share(where, d, two_send, two_recv, axis_two))
        from_three.append(share(where, d, three_send, three_recv, axis_three))
        from_core.append(share(where, d, sib_send, sib_recv, sibling))
    x_two, y_two = x + (1 - c) * (1 - 2 * x), y + c * (1 - 2 * y)
    for d in range(zs):
        from_two[d].wait_recv()
        where = (y_two, x_two, lax.rem(z - d + zs, zs))
        from_three.append(share(where, zs + d, three_send, three_recv, axis_three))
        from_core.append(share(where, zs + d, sib_send, sib_recv, sibling))
    x_three, y_three = x + c * (1 - 2 * x), y + (1 - c) * (1 - 2 * y)
    for d in range(2 * zs):
        from_three[d].wait_recv()
        zi = lax.rem(z - d + 2 * zs, zs)
        where = (y_three, x_three, zi) if d < zs else (1 - y, 1 - x, zi)
        from_core.append(share(where, 2 * zs + d, sib_send, sib_recv, sibling))
    for copy in from_core:
        copy.wait_recv()
    for load in loads[6:]:
        load.wait()

    count = 4 * zs * padded
    gate_act, up_act = 0.0, 0.0
    for yi in range(2):
        taken = rows[yi, :, :, :, :, :half].reshape(count, half)
        depth = slice(yi * half, (yi + 1) * half)
        gate_act += jnp.dot(taken, gate_w[depth], preferred_element_type=jnp.float32)
        up_act += jnp.dot(taken, up_w[depth], preferred_element_type=jnp.float32)
    hidden = (jax.nn.silu(gate_act) * up_act).astype(jnp.bfloat16)
    coded = rows[0, :, :, :, :, half:].reshape(count, -1).astype(jnp.float32)
    lane = lax.broadcasted_iota(jnp.int32, coded.shape, 1)
    named = (lane == ep) | (lane == ep + experts)
    weight = jnp.sum(jnp.where(named, coded, 0.0), axis=1, keepdims=True)

    def piece(yi, ci):
        columns = pl.ds(pl.multiple_of(yi * half + ci * quarter, quarter), quarter)
        result = jnp.dot(hidden, down_w[:, columns], preferred_element_type=jnp.float32)
        return (result * weight).reshape(2, zs, 2, padded, quarter)

    halves = []
    some = (slice(None), slice(None), slice(None), pl.ds(0, live), slice(None))
    for yi in range(2):
        for_sib[yi] = piece(yi, 1 - c).astype(jnp.bfloat16)
        halves.append(
            send(
                for_sib.at[(yi,) + some],
                from_sib.at[(yi,) + some],
                red_send.at[yi],
                red_recv.at[yi],
                sibling,
            )
        )
    for yi in range(2):
        own[yi] = piece(yi, c)
    for copy in halves:
        copy.wait_recv()

    one = y + c * (x - y)
    two = x + c * (y - x)

    def summed(fi, si, zi):
        yi, xi = fi + c * (si - fi), si + c * (fi - si)
        return own[yi, xi, zi] + from_sib[yi, xi, zi].astype(jnp.float32)

    order = [lax.rem(z + d, zs) for d in list(range(1, zs)) + [0]]
    cut = (slice(None), pl.ds(0, live), slice(None))
    to_first, to_second, along_z = [], [], []
    for j, si in enumerate((1 - two, two)):
        for i, zi in enumerate(order):
            stage_a[si, zi] = summed(1 - one, si, zi).astype(jnp.bfloat16)
            at = (si, zi) + cut
            slot = j * zs + i
            to_first.append(
                send(stage_a.at[at], recv_a.at[at], a_send.at[slot], a_recv.at[slot], axis_three)
            )
    for i, zi in enumerate(order):
        to_first[i].wait_recv()
        stage_b[zi] = (
            summed(one, 1 - two, zi) + recv_a[1 - two, zi].astype(jnp.float32)
        ).astype(jnp.bfloat16)
        at = (zi,) + cut
        to_second.append(
            send(stage_b.at[at], recv_b.at[at], b_send.at[i], b_recv.at[i], axis_two)
        )
    for i, zi in enumerate(order):
        to_first[zs + i].wait_recv()
        to_second[i].wait_recv()
        kept = (
            summed(one, two, zi)
            + recv_a[two, zi].astype(jnp.float32)
            + recv_b[zi].astype(jnp.float32)
        )
        if i < zs - 1:
            stage_c[zi] = kept.astype(jnp.bfloat16)
            along_z.append(
                send(
                    stage_c.at[(zi,) + cut],
                    recv_c.at[(i,) + cut],
                    red_send.at[3 + i],
                    red_recv.at[3 + i],
                    device(zi, x, c, y),
                )
            )
    total = kept
    for i in range(zs - 1):
        along_z[i].wait_recv()
        total = total + recv_c[i].astype(jnp.float32)
    stage_d[...] = total
    last = send(stage_d.at[1 - c], recv_d, red_send.at[2], red_recv.at[2], sibling)
    near = pl.ds(pl.multiple_of(c * quarter, quarter), quarter)
    far = pl.ds(pl.multiple_of((1 - c) * quarter, quarter), quarter)
    out_ref[:, near] = (resid[:, near] + stage_d[c, :tokens]).astype(out_ref.dtype)
    last.wait_recv()
    out_ref[:, far] = (resid[:, far] + recv_d[:tokens]).astype(out_ref.dtype)
    for copy in pending:
        copy.wait_send()


def dense_shards(
    hidden_in,
    attn_gain,
    w_query,
    w_key,
    w_value,
    break_bias,
    key_cache,
    value_cache,
    lengths,
    w_out,
    ffn_gain,
    route_ids,
    route_scores,
    expert_gate,
    expert_up,
    expert_down,
):
    tokens, half = hidden_in.shape
    padded = tokens + -tokens % 16
    width = 2 * half
    experts = lax.axis_size("ep")
    heads = break_bias.shape[0]
    zs = experts // 4
    extra = 2 * experts + -2 * experts % 128
    blocks = (2, zs, 2, padded, half // 2)
    bf16, f32 = jnp.bfloat16, jnp.float32
    vmem = pl.BlockSpec(memory_space=pltpu.VMEM)
    smem = pl.BlockSpec(memory_space=pltpu.SMEM)
    hbm = pl.BlockSpec(memory_space=pl.ANY)
    dma = pltpu.SemaphoreType.DMA
    columns_in, span = key_cache.shape[1:]
    sizes = (tokens, padded, zs, width, half, experts, heads)
    new_shape = jax.ShapeDtypeStruct((tokens, columns_in), bf16)
    pairs = [4, zs - 1, zs, 2 * zs, 4 * zs, 3 + zs, 2 * zs, zs]
    results = pl.pallas_call(
        functools.partial(layer_kernel, sizes),
        out_shape=(jax.ShapeDtypeStruct((tokens, half), bf16), new_shape, new_shape),
        in_specs=[vmem, vmem, smem, smem, vmem, vmem, vmem] + [hbm] * 9,
        out_specs=(vmem, vmem, vmem),
        scratch_shapes=[
            pltpu.VMEM((3,) + w_query.shape, bf16),
            pltpu.VMEM(key_cache.shape, bf16),
            pltpu.VMEM(value_cache.shape, bf16),
            pltpu.VMEM((2,) + w_out.shape, bf16),
            pltpu.VMEM(expert_gate.shape[1:], bf16),
            pltpu.VMEM(expert_up.shape[1:], bf16),
            pltpu.VMEM(expert_down.shape[1:], bf16),
            pltpu.VMEM((2, tokens, half), bf16),
            pltpu.VMEM((padded, width), bf16),
            pltpu.VMEM((heads, padded, span), f32),
            pltpu.VMEM((padded, span), jnp.int32),
            pltpu.VMEM((heads, padded, span), f32),
            pltpu.VMEM((extra, 128), f32),
            pltpu.VMEM((2, padded, columns_in), bf16),
            pltpu.VMEM((tokens, half), f32),
            pltpu.VMEM((2, 2, zs, 2, padded, half + extra), bf16),
            pltpu.VMEM((2,) + blocks, f32),
            pltpu.VMEM((2,) + blocks, bf16),
            pltpu.VMEM((2,) + blocks, bf16),
            pltpu.VMEM(blocks, bf16),
            pltpu.VMEM(blocks, bf16),
            pltpu.VMEM(blocks[1:], bf16),
            pltpu.VMEM(blocks[1:], bf16),
            pltpu.VMEM(blocks[1:], bf16),
            pltpu.VMEM((zs - 1,) + blocks[2:], bf16),
            pltpu.VMEM(blocks[2:], f32),
            pltpu.VMEM(blocks[3:], f32),
            dma((9,)),
        ]
        + [dma((count,)) for count in pairs for _ in range(2)],
        compiler_params=pltpu.CompilerParams(
            collective_id=0, has_side_effects=True, vmem_limit_bytes=60 * 1024 * 1024
        ),
    )(
        hidden_in,
        attn_gain[None, :],
        break_bias,
        lengths,
        ffn_gain[None, :],
        route_ids.T,
        route_scores.T,
        w_query,
        w_key,
        w_value,
        key_cache,
        value_cache,
        w_out,
        expert_gate,
        expert_up,
        expert_down,
    )
    return pl.pallas_call(
        hand_on,
        out_shape=tuple(jax.ShapeDtypeStruct(r.shape, r.dtype) for r in results),
        in_specs=[vmem] * 3,
        out_specs=(vmem, vmem, vmem),
    )(*results)


def solution(mesh):
    ep_size, tp_size = mesh.shape["ep"], mesh.shape["tp"]
    fits = tp_size == 2 and ep_size % 4 == 0 and 8 <= ep_size <= 16
    body = dense_shards if fits else shards
    return jax.shard_map(
        body,
        mesh=mesh,
        in_specs=(
            P("ep", "tp"),
            P(),
            P("tp", None),
            P("tp", None),
            P("tp", None),
            P("tp"),
            P("ep", "tp", None),
            P("ep", "tp", None),
            P("ep"),
            P("tp", None),
            P(),
            P("ep", None),
            P("ep", None),
            P("ep", None, "tp"),
            P("ep", None, "tp"),
            P("ep", "tp", None),
        ),
        out_specs=(P("ep", "tp"), P("ep", "tp"), P("ep", "tp")),
        check_vma=False,
    )
```
